32 devices in a mesh: sp: 8 (over z, y), tp: 4 (over x, core).
Axes of the slice: x: 2, y: 2, z: 4, core: 2. Of those that a mesh axis runs over, the one named last changes fastest.
Arguments:
- residual: bfloat16 [5120, 2048], P(('sp', 'tp')), may hold values from -6 to 6
- small_value_inputs: bfloat16 [5120, 1024], P('sp', 'tp'), may hold values from -6 to 6
- large_value_inputs: bfloat16 [5120, 1024], P('sp', 'tp'), may hold values from -6 to 6
- small_gate_inputs: bfloat16 [5120, 1024], P('sp', 'tp'), may hold values from -6 to 6
- large_gate_inputs: bfloat16 [5120, 1024], P('sp', 'tp'), may hold values from -6 to 6
- state_projections: bfloat16 [5120, 4, 128], P('sp'), may hold values from -6 to 6
- small_step_inputs: bfloat16 [5120, 16], P('sp', 'tp'), may hold values from -2.5 to 2.5
- large_step_inputs: bfloat16 [5120, 8], P('sp', 'tp'), may hold values from -2.5 to 2.5
- small_decay_offsets: float32 [5120, 16], P('sp', 'tp'), may hold values from -1.4 to 0
- large_decay_offsets: float32 [5120, 8], P('sp', 'tp'), may hold values from -1.4 to 0
- small_decay_rates: float32 [16], P('tp'), may hold values from -11.1 to -3.1
- large_decay_rates: float32 [8], P('tp'), may hold values from -11.1 to -3.1
- small_filter_taps: bfloat16 [4, 1024], P(None, 'tp'), may hold values from -3 to 3
- large_filter_taps: bfloat16 [4, 1024], P(None, 'tp'), may hold values from -3 to 3
- state_filter_taps: bfloat16 [4, 4, 128], replicated, may hold values from -3 to 3
- small_head_gains: float32 [1024], P('tp'), may hold values from 0.1 to 1.9
- large_head_gains: float32 [1024], P('tp'), may hold values from 0.1 to 1.9
- small_output_projection: bfloat16 [1024, 2048], P('tp'), may hold values from -0.125 to 0.125
- large_output_projection: bfloat16 [1024, 2048], P('tp'), may hold values from -0.125 to 0.125
- channel_norm_gain: float32 [2048], replicated, may hold values from 0.1 to 1.9
- gate_matrix: bfloat16 [2048, 5632], P('sp', 'tp'), may hold values from -0.125 to 0.125
- up_matrix: bfloat16 [2048, 5632], P('sp', 'tp'), may hold values from -0.125 to 0.125
- down_matrix: bfloat16 [5632, 2048], P('tp', 'sp'), may hold values from -0.078125 to 0.078125
Outputs:
- layer_out: bfloat16 [5120, 2048], P(('sp', 'tp'))
The draws below stay inside these ranges and needn't reach their ends.
All inputs are finite; a program needn't handle non-finite values.
Results may differ from the reference program's by a relative error of at most 0.015.
Values may be sent and summed in bfloat16 or wider, within the bound.
A program may use at most 64 MiB of HBM per device.

```python
import jax
import jax.numpy as jnp
from jax import lax

D = 2048
FF = 5632
SMALL_HEADS = 16
LARGE_HEADS = 8
STATE = 128
BLOCK = 64
CONV = 4
TOK_DEV = 640
TOKENS = 5120
W1 = 1024
W2 = 1024
N_TP = 4


def step_draw(key, head_outputs):
    first, second = jax.random.split(key)
    blocks = TOKENS // TOK_DEV
    offset = jax.random.uniform(first, (blocks, 1, head_outputs), jnp.float32, -1.0, 1.0)
    base = 0.5 * jax.random.truncated_normal(second, -3.0, 3.0, (blocks, TOK_DEV, head_outputs), jnp.float32)
    return (base + offset).reshape(TOKENS, head_outputs).astype(jnp.bfloat16)


def rate_draw(key, head_outputs):
    first, second, third = jax.random.split(key, 3)
    quick = jax.random.uniform(first, (head_outputs,), jnp.float32) < 0.5
    slow_rate = jax.random.uniform(second, (head_outputs,), jnp.float32, 0.2, 0.8) / (0.75 * TOKENS)
    fast_rate = 1.0 / (0.75 * jax.random.uniform(third, (head_outputs,), jnp.float32, 30.0, 100.0))
    return jnp.log(jnp.where(quick, fast_rate, slow_rate)).astype(jnp.float32)


def decay_offset_sample(key, head_outputs):
    first, second = jax.random.split(key)
    places = jax.random.randint(first, (2, head_outputs), 0, TOKENS)
    sizes = jnp.log(jax.random.uniform(second, (2, head_outputs), jnp.float32, 0.5, 0.8))
    hit = jnp.arange(TOKENS, dtype=jnp.int32)[:, None, None] == places[None, :, :]
    return jnp.sum(jnp.where(hit, sizes[None, :, :], 0.0), axis=1).astype(jnp.float32)


def draw_small_step_inputs(key, part):
    return step_draw(jax.random.fold_in(key, 11), SMALL_HEADS)


def draw_large_step_inputs(key, part):
    return step_draw(jax.random.fold_in(key, 12), LARGE_HEADS)


def draw_small_decay_rates(key, part):
    return rate_draw(jax.random.fold_in(key, 21), SMALL_HEADS)


def draw_large_decay_rates(key, part):
    return rate_draw(jax.random.fold_in(key, 22), LARGE_HEADS)


def draw_small_decay_offsets(key, part):
    return decay_offset_sample(jax.random.fold_in(key, 31), SMALL_HEADS)


def draw_large_decay_offsets(key, part):
    return decay_offset_sample(jax.random.fold_in(key, 32), LARGE_HEADS)


def steps_of(own_key, dims, cuts, low, largest):
    level = 1.0
    for position, blocks in cuts:
        heights = jax.random.uniform(jax.random.fold_in(jax.random.fold_in(own_key, 6), position), (blocks,), jnp.float32, low / len(cuts), largest / len(cuts))
        level = level * jnp.repeat(jnp.exp(heights), dims[position] // blocks).reshape((-1,) + (1,) * (len(dims) - 1 - position))
    return level


def normal_values(stream_key, shape, scale, bound, cuts=(), kind=jnp.bfloat16):
    result = jax.random.normal(stream_key, shape, jnp.float32) * scale
    if len(cuts) > 0:
        result = steps_of(stream_key, shape, cuts, -0.22, 0.18) * result
    return jnp.clip(result, min=-bound, max=bound).astype(kind)


def setup_inputs(seed: int = 0) -> dict:
    arg_keys = jax.random.split(jax.random.key(seed), 24)
    return {
        "residual": normal_values(arg_keys[0], (TOKENS, D), 1.0, 6.0, ((0, 32),)),
        "small_value_inputs": normal_values(arg_keys[1], (TOKENS, W1), 1.0, 6.0, ((0, 8), (1, 4))),
        "large_value_inputs": normal_values(arg_keys[2], (TOKENS, W2), 1.0, 6.0, ((0, 8), (1, 4))),
        "small_gate_inputs": normal_values(arg_keys[3], (TOKENS, W1), 1.0, 6.0, ((0, 8), (1, 4))),
        "large_gate_inputs": normal_values(arg_keys[4], (TOKENS, W2), 1.0, 6.0, ((0, 8), (1, 4))),
        "state_projections": normal_values(arg_keys[5], (TOKENS, 4, STATE), 1.0, 6.0, ((0, 8),)),
        "small_step_inputs": draw_small_step_inputs(jax.random.fold_in(arg_keys[23], 71), 0),
        "large_step_inputs": draw_large_step_inputs(jax.random.fold_in(arg_keys[23], 71), 0),
        "small_decay_offsets": draw_small_decay_offsets(jax.random.fold_in(arg_keys[23], 71), 0),
        "large_decay_offsets": draw_large_decay_offsets(jax.random.fold_in(arg_keys[23], 71), 0),
        "small_decay_rates": draw_small_decay_rates(jax.random.fold_in(arg_keys[23], 71), 0),
        "large_decay_rates": draw_large_decay_rates(jax.random.fold_in(arg_keys[23], 71), 0),
        "small_filter_taps": normal_values(arg_keys[12], (CONV, W1), CONV ** -0.5, 3.0, ((1, 4),)),
        "large_filter_taps": normal_values(arg_keys[13], (CONV, W2), CONV ** -0.5, 3.0, ((1, 4),)),
        "state_filter_taps": normal_values(arg_keys[14], (CONV, 4, STATE), CONV ** -0.5, 3.0),
        "small_head_gains": jnp.clip(1.0 + 0.18 * jax.random.normal(arg_keys[15], (W1,), jnp.float32), 0.1, 1.9),
        "large_head_gains": jnp.clip(1.0 + 0.18 * jax.random.normal(arg_keys[16], (W2,), jnp.float32), 0.1, 1.9),
        "small_output_projection": normal_values(arg_keys[17], (W1, D), (W1 + W2) ** -0.5, 0.125, ((0, 4),)),
        "large_output_projection": normal_values(arg_keys[18], (W2, D), (W1 + W2) ** -0.5, 0.125, ((0, 4),)),
        "channel_norm_gain": jnp.clip(1.0 + 0.18 * jax.random.normal(arg_keys[19], (D,), jnp.float32), 0.1, 1.9),
        "gate_matrix": normal_values(arg_keys[20], (D, FF), D ** -0.5, 0.125, ((0, 8), (1, 4))),
        "up_matrix": normal_values(arg_keys[21], (D, FF), D ** -0.5, 0.125, ((0, 8), (1, 4))),
        "down_matrix": normal_values(arg_keys[22], (FF, D), FF ** -0.5, 0.078125, ((0, 4), (1, 8))),
    }


HIGH = lax.Precision.HIGHEST
head_eps = 1e-05
row_eps = 1e-06

def rounded(value):
    return lax.optimization_barrier(value.astype(jnp.bfloat16)).astype(jnp.float32)

def causal_conv(series, prior_tokens, filter_taps):
    width = filter_taps.shape[0]
    length = series.shape[0]
    padded = jnp.concatenate([prior_tokens.astype(jnp.float32), series.astype(jnp.float32)], axis=0)
    total = jnp.zeros(series.shape, jnp.float32)
    for offset in range(width):
        total = total + filter_taps[offset].astype(jnp.float32)[None, :] * padded[offset:offset + length]
    return jax.nn.silu(total)

def block_scan(driven, decay_logarithm, key_vectors, read_vectors, state):
    length, head_outputs, size = driven.shape
    blocks = length // BLOCK
    mask = jnp.tril(jnp.ones((BLOCK, BLOCK), dtype=bool))[:, :, None]

    def advance(carry, pieces):
        values, decays, key_rows, read_rows = pieces
        within = jnp.cumsum(decays, axis=0)
        spread = within[:, None, :] - within[None, :, :]
        weights = jnp.where(mask, jnp.exp(jnp.where(mask, spread, 0.0)), 0.0)
        scores = jnp.dot(read_rows, key_rows.T, precision=HIGH)
        inner = jnp.einsum('ls,lsh,shp->lhp', scores, weights, values, precision=HIGH)
        carried = jnp.einsum('ln,hpn,lh->lhp', read_rows, carry, jnp.exp(within), precision=HIGH)
        tail = jnp.exp(within[-1][None, :] - within)
        fresh = jnp.einsum('ln,lh,lhp->hpn', key_rows, tail, values, precision=HIGH)
        return (carry * jnp.exp(within[-1])[:, None, None] + fresh, inner + carried)
    pieces = (driven.reshape(blocks, BLOCK, head_outputs, size), decay_logarithm.reshape(blocks, BLOCK, head_outputs), key_vectors.reshape(blocks, BLOCK, key_vectors.shape[1]), read_vectors.reshape(blocks, BLOCK, read_vectors.shape[1]))
    final, outs = lax.scan(advance, state, pieces)
    return (final, outs.reshape(length, head_outputs, size))

def heads_per_group(input_rows, gate_inputs, step_inputs, decay_offsets, decay_rates, filter_taps, head_gains, key_vectors, read_vectors):
    length, width = input_rows.shape
    head_outputs = decay_rates.shape[0]
    size = width // head_outputs
    prior_tokens = jnp.zeros((filter_taps.shape[0] - 1, width), jnp.bfloat16)
    conv_values = causal_conv(input_rows, prior_tokens, filter_taps)
    step_amount = jax.nn.softplus(step_inputs.astype(jnp.float32))
    decay_logarithm = -jnp.exp(decay_rates)[None, :] * step_amount + decay_offsets
    driven = conv_values.reshape(length, head_outputs, size) * step_amount[:, :, None]
    start_state = jnp.zeros((head_outputs, size, key_vectors.shape[1]), jnp.float32)
    _, scan_out = block_scan(driven, decay_logarithm, key_vectors, read_vectors, start_state)
    gated = scan_out * jax.nn.silu(gate_inputs.reshape(length, head_outputs, size).astype(jnp.float32))
    scale = lax.rsqrt(lax.optimization_barrier(jnp.mean(gated * gated, axis=-1, keepdims=True)) + head_eps)
    normed = gated * scale * head_gains.reshape(head_outputs, size).astype(jnp.float32)
    return normed.reshape(length, width).astype(jnp.bfloat16)

def row_norm(rows, gain):
    wide = rows.astype(jnp.float32)
    scale = lax.rsqrt(lax.optimization_barrier(jnp.mean(wide * wide, axis=-1, keepdims=True)) + row_eps)
    return (wide * scale * gain[None, :]).astype(jnp.bfloat16)

def reference(residual, small_value_inputs, large_value_inputs, small_gate_inputs, large_gate_inputs, state_projections, small_step_inputs, large_step_inputs, small_decay_offsets, large_decay_offsets, small_decay_rates, large_decay_rates, small_filter_taps, large_filter_taps, state_filter_taps, small_head_gains, large_head_gains, small_output_projection, large_output_projection, channel_norm_gain, gate_matrix, up_matrix, down_matrix):
    length = residual.shape[0]
    planes = state_projections.shape[1] * state_projections.shape[2]
    flat = state_projections.reshape(length, planes)
    flat_taps = state_filter_taps.reshape(state_filter_taps.shape[0], planes)
    prior_tokens = jnp.zeros((state_filter_taps.shape[0] - 1, planes), jnp.bfloat16)
    convolved_state_maps = causal_conv(flat, prior_tokens, flat_taps).reshape(length, state_projections.shape[1], state_projections.shape[2])
    small_head_outputs = heads_per_group(small_value_inputs, small_gate_inputs, small_step_inputs, small_decay_offsets, small_decay_rates, small_filter_taps, small_head_gains, convolved_state_maps[:, 0], convolved_state_maps[:, 1])
    large_head_outputs = heads_per_group(large_value_inputs, large_gate_inputs, large_step_inputs, large_decay_offsets, large_decay_rates, large_filter_taps, large_head_gains, convolved_state_maps[:, 2], convolved_state_maps[:, 3])
    slice_small = W1 // N_TP
    slice_large = W2 // N_TP
    mixed = jnp.zeros((length, D), jnp.float32)
    for part in range(N_TP):
        term = jnp.dot(small_head_outputs[:, part * slice_small:(part + 1) * slice_small], small_output_projection[part * slice_small:(part + 1) * slice_small], preferred_element_type=jnp.float32)
        term = term + jnp.dot(large_head_outputs[:, part * slice_large:(part + 1) * slice_large], large_output_projection[part * slice_large:(part + 1) * slice_large], preferred_element_type=jnp.float32)
        mixed = mixed + rounded(term)
    middle = (residual.astype(jnp.float32) + mixed).astype(jnp.bfloat16)
    normed = row_norm(middle, channel_norm_gain)
    gate = jnp.dot(normed, gate_matrix, preferred_element_type=jnp.float32)
    up = jnp.dot(normed, up_matrix, preferred_element_type=jnp.float32)
    hidden = (jax.nn.silu(gate) * up).astype(jnp.bfloat16)
    slice_units = FF // N_TP
    down = jnp.zeros((length, D), jnp.float32)
    for part in range(N_TP):
        down = down + rounded(jnp.dot(hidden[:, part * slice_units:(part + 1) * slice_units], down_matrix[part * slice_units:(part + 1) * slice_units], preferred_element_type=jnp.float32))
    return (middle.astype(jnp.float32) + down).astype(jnp.bfloat16)
```

```python
import jax
import jax.numpy as jnp
from jax import lax
from jax.sharding import PartitionSpec as P

HIGH = lax.Precision.HIGHEST
head_eps = 1e-05
row_eps = 1e-06
BF = jnp.bfloat16
F32 = jnp.float32


def ring_order(n):
    ys = 1
    while ys * ys * 4 <= n:
        ys *= 2
    zs = n // ys
    if ys * zs != n or ys < 2 or zs % 2:
        return list(range(n))
    walk = []
    for z in range(zs):
        row = list(range(1, ys))
        walk += [z * ys + y for y in (row if z % 2 == 0 else row[::-1])]
    return walk + [z * ys for z in reversed(range(zs))]


def causal_conv(series, prior, taps):
    width, length = taps.shape[0], series.shape[0]
    padded = jnp.concatenate([prior, series], axis=0).astype(F32)
    total = jnp.zeros(series.shape, F32)
    for offset in range(width):
        total = total + taps[offset].astype(F32)[None, :] * padded[offset : offset + length]
    return jax.nn.silu(total)


def local_heads(conv_values, step, within, keys, reads):
    length, width = conv_values.shape
    heads = step.shape[1]
    size = width // heads
    driven = conv_values.reshape(length, heads, size) * step[:, :, None]
    scores = lax.dot_general(reads, keys, (((1,), (1,)), ((), ())), preferred_element_type=F32)
    mask = jnp.tril(jnp.ones((length, length), dtype=bool))
    outs, finals = [], []
    for h in range(heads):
        own = within[:, h]
        spread = jnp.where(mask, own[:, None] - own[None, :], 0.0)
        mixing = jnp.where(mask, jnp.exp(spread) * scores, 0.0).astype(BF)
        value = driven[:, h]
        outs.append(jnp.dot(mixing, value.astype(BF), preferred_element_type=F32))
        late = (value * jnp.exp(own[-1] - own)[:, None]).astype(BF)
        finals.append(
            lax.dot_general(late, keys, (((0,), (0,)), ((), ())), preferred_element_type=F32)
        )
    return outs, jnp.concatenate(finals, axis=0)


def finish_heads(outs, incoming, within, reads, gate_inputs, gains):
    size = outs[0].shape[1]
    done = []
    carried = lax.dot_general(
        reads, incoming.astype(BF), (((1,), (1,)), ((), ())), preferred_element_type=F32
    )
    for h, local in enumerate(outs):
        cols = slice(h * size, (h + 1) * size)
        scan_out = local + carried[:, cols] * jnp.exp(within[:, h])[:, None]
        gated = scan_out * jax.nn.silu(gate_inputs[:, cols].astype(F32))
        scale = lax.rsqrt(jnp.mean(gated * gated, axis=-1, keepdims=True) + head_eps)
        done.append((gated * scale * gains[cols][None, :]).astype(BF))
    return jnp.concatenate(done, axis=1)


def row_norm(rows, gain):
    wide = rows.astype(F32)
    scale = lax.rsqrt(jnp.mean(wide * wide, axis=-1, keepdims=True) + row_eps)
    return (wide * scale * gain[None, :]).astype(BF)


def ring_gather(own):
    n = lax.axis_size("sp")
    order = ring_order(n)
    place = [order.index(i) for i in range(n)]
    me = lax.axis_index("sp")
    at = jnp.asarray(place, jnp.int32)[me]
    owners = jnp.asarray(order, jnp.int32)
    ahead = [(order[i], order[(i + 1) % n]) for i in range(n)]
    back = [(b, a) for a, b in ahead]
    rows = own.shape[0]
    whole = jnp.zeros((n * rows,) + own.shape[1:], own.dtype)
    whole = lax.dynamic_update_slice(whole, own, (me * rows, 0))
    up = down = own
    half = n // 2
    for k in range(1, half + 1):
        from_up = owners[(at - k) % n] * rows
        from_down = owners[(at + k) % n] * rows
        if 2 * k == n:
            cut = rows // 2
            up, down = up[:cut], down[cut:]
            from_down = from_down + cut
        up = lax.ppermute(up, "sp", ahead)
        down = lax.ppermute(down, "sp", back)
        whole = lax.dynamic_update_slice(whole, up, (from_up, 0))
        whole = lax.dynamic_update_slice(whole, down, (from_down, 0))
    return whole


def on_device(
    residual,
    small_value_inputs,
    large_value_inputs,
    small_gate_inputs,
    large_gate_inputs,
    state_projections,
    small_step_inputs,
    large_step_inputs,
    small_decay_offsets,
    large_decay_offsets,
    small_decay_rates,
    large_decay_rates,
    small_filter_taps,
    large_filter_taps,
    state_filter_taps,
    small_head_gains,
    large_head_gains,
    small_output_projection,
    large_output_projection,
    channel_norm_gain,
    gate_matrix,
    up_matrix,
    down_matrix,
):
    n = lax.axis_size("sp")
    me = lax.axis_index("sp")
    margin = state_filter_taps.shape[0] - 1
    length, w1 = small_value_inputs.shape
    w2 = large_value_inputs.shape[1]
    state = state_projections.shape[2]
    planes = state_projections.shape[1] * state
    units = gate_matrix.shape[1]
    flat = state_projections.reshape(length, planes)
    series = jnp.concatenate([small_value_inputs, large_value_inputs, flat], axis=1)
    prior = lax.ppermute(
        series[length - margin :], "sp", [(i, i + 1) for i in range(n - 1)]
    )
    pack = jnp.concatenate([gate_matrix, up_matrix, down_matrix.T], axis=1)
    pack, prior = lax.optimization_barrier((pack, prior))
    whole = ring_gather(pack)

    taps = jnp.concatenate(
        [small_filter_taps, large_filter_taps, state_filter_taps.reshape(margin + 1, planes)], axis=1
    )
    conv = causal_conv(series, prior, taps)
    maps = conv[:, w1 + w2 :].astype(BF)
    keys1, reads1, keys2, reads2 = (maps[:, i * state : (i + 1) * state] for i in range(4))

    heads1 = small_decay_rates.shape[0]
    step = jax.nn.softplus(
        jnp.concatenate([small_step_inputs, large_step_inputs], axis=1).astype(F32)
    )
    rates = jnp.concatenate([small_decay_rates, large_decay_rates])
    offsets = jnp.concatenate([small_decay_offsets, large_decay_offsets], axis=1)
    log_decay = -jnp.exp(rates)[None, :] * step + offsets
    lower = jnp.tril(jnp.ones((length, length), F32))
    within = jnp.dot(lower, log_decay, precision=HIGH)

    outs1, final1 = local_heads(conv[:, :w1], step[:, :heads1], within[:, :heads1], keys1, reads1)
    outs2, final2 = local_heads(
        conv[:, w1 : w1 + w2], step[:, heads1:], within[:, heads1:], keys2, reads2
    )
    heads = rates.shape[0]
    total = jnp.exp(within[-1])
    sizes = [w1 // heads1] * heads1 + [w2 // (heads - heads1)] * (heads - heads1)
    row = jnp.pad(total[None, :], ((0, 15), (0, state - heads)))
    sent = jnp.concatenate([final1, final2, row], axis=0).astype(BF)
    gathered = lax.all_gather(sent, "sp").astype(F32)
    carry = jnp.zeros((w1 + w2, state), F32)
    for hop in range(n - 1):
        factor = jnp.concatenate(
            [
                jnp.broadcast_to(gathered[hop, w1 + w2, h], (sizes[h], 1))
                for h in range(heads)
            ],
            axis=0,
        )
        carry = jnp.where(hop < me, carry * factor + gathered[hop, : w1 + w2], carry)

    heads_small = finish_heads(
        outs1, carry[:w1], within[:, :heads1], reads1, small_gate_inputs, small_head_gains
    )
    heads_large = finish_heads(
        outs2, carry[w1:], within[:, heads1:], reads2, large_gate_inputs, large_head_gains
    )
    mixed = lax.psum_scatter(
        (
            jnp.dot(heads_small, small_output_projection, preferred_element_type=F32)
            + jnp.dot(heads_large, large_output_projection, preferred_element_type=F32)
        ).astype(BF),
        "tp",
        scatter_dimension=0,
        tiled=True,
    ).astype(F32)
    middle = (residual.astype(F32) + mixed).astype(BF)
    normed = row_norm(middle, channel_norm_gain)
    normed_all = lax.all_gather(normed, "tp", axis=0, tiled=True)
    gate = jnp.dot(normed_all, whole[:, :units], preferred_element_type=F32)
    up = jnp.dot(normed_all, whole[:, units : 2 * units], preferred_element_type=F32)
    hidden = (jax.nn.silu(gate) * up).astype(BF)
    partial = lax.dot_general(
        hidden, whole[:, 2 * units :], (((1,), (1,)), ((), ())), preferred_element_type=F32
    )
    down = lax.psum_scatter(
        partial.astype(BF), "tp", scatter_dimension=0, tiled=True
    ).astype(F32)
    return (middle.astype(F32) + down).astype(BF)


def solution(mesh):
    in_specs = (
        P(("sp", "tp"), None),
        P("sp", "tp"),
        P("sp", "tp"),
        P("sp", "tp"),
        P("sp", "tp"),
        P("sp", None, None),
        P("sp", "tp"),
        P("sp", "tp"),
        P("sp", "tp"),
        P("sp", "tp"),
        P("tp"),
        P("tp"),
        P(None, "tp"),
        P(None, "tp"),
        P(),
        P("tp"),
        P("tp"),
        P("tp", None),
        P("tp", None),
        P(),
        P("sp", "tp"),
        P("sp", "tp"),
        P("tp", "sp"),
    )
    return jax.shard_map(
        on_device,
        mesh=mesh,
        in_specs=in_specs,
        out_specs=P(("sp", "tp"), None),
        check_vma=False,
    )
```

```python
import jax
import jax.numpy as jnp
from jax import lax
from jax.sharding import PartitionSpec as P


HIGH = lax.Precision.HIGHEST
head_eps = 1e-05
row_eps = 1e-06
BF = jnp.bfloat16
F32 = jnp.float32


def ring_order(n):
    ys = 1
    while ys * ys * 4 <= n:
        ys *= 2
    zs = n // ys
    if ys * zs != n or ys < 2 or zs % 2:
        return list(range(n))
    walk = []
    for z in range(zs):
        row = list(range(1, ys))
        walk += [z * ys + y for y in (row if z % 2 == 0 else row[::-1])]
    return walk + [z * ys for z in reversed(range(zs))]


def causal_conv(series, prior, taps):
    width, length = taps.shape[0], series.shape[0]
    padded = jnp.concatenate([prior, series], axis=0).astype(F32)
    total = jnp.zeros(series.shape, F32)
    for offset in range(width):
        total = total + taps[offset].astype(F32)[None, :] * padded[offset : offset + length]
    return jax.nn.silu(total)


def local_heads(conv_values, step, within, keys, reads):
    length, width = conv_values.shape
    heads = step.shape[1]
    size = width // heads
    driven = conv_values.reshape(length, heads, size) * step[:, :, None]
    scores = lax.dot_general(reads, keys, (((1,), (1,)), ((), ())), preferred_element_type=F32)
    mask = jnp.tril(jnp.ones((length, length), dtype=bool))
    outs, finals = [], []
    for h in range(heads):
        own = within[:, h]
        spread = jnp.where(mask, own[:, None] - own[None, :], 0.0)
        mixing = jnp.where(mask, jnp.exp(spread) * scores, 0.0).astype(BF)
        value = driven[:, h]
        outs.append(jnp.dot(mixing, value.astype(BF), preferred_element_type=F32))
        late = (value * jnp.exp(own[-1] - own)[:, None]).astype(BF)
        finals.append(
            lax.dot_general(late, keys, (((0,), (0,)), ((), ())), preferred_element_type=F32)
        )
    return outs, jnp.concatenate(finals, axis=0)


def finish_heads(outs, incoming, within, reads, gate_inputs, gains):
    size = outs[0].shape[1]
    done = []
    carried = lax.dot_general(
        reads, incoming.astype(BF), (((1,), (1,)), ((), ())), preferred_element_type=F32
    )
    for h, local in enumerate(outs):
        cols = slice(h * size, (h + 1) * size)
        scan_out = local + carried[:, cols] * jnp.exp(within[:, h])[:, None]
        gated = scan_out * jax.nn.silu(gate_inputs[:, cols].astype(F32))
        scale = lax.rsqrt(jnp.mean(gated * gated, axis=-1, keepdims=True) + head_eps)
        done.append((gated * scale * gains[cols][None, :]).astype(BF))
    return jnp.concatenate(done, axis=1)


def row_norm(rows, gain):
    wide = rows.astype(F32)
    scale = lax.rsqrt(jnp.mean(wide * wide, axis=-1, keepdims=True) + row_eps)
    return (wide * scale * gain[None, :]).astype(BF)


def ring_gather(own):
    n = lax.axis_size("sp")
    order = ring_order(n)
    place = [order.index(i) for i in range(n)]
    me = lax.axis_index("sp")
    at = jnp.asarray(place, jnp.int32)[me]
    owners = jnp.asarray(order, jnp.int32)
    ahead = [(order[i], order[(i + 1) % n]) for i in range(n)]
    back = [(b, a) for a, b in ahead]
    rows = own.shape[0]
    whole = jnp.zeros((n * rows,) + own.shape[1:], own.dtype)
    whole = lax.dynamic_update_slice(whole, own, (me * rows, 0))
    up = down = own
    half = n // 2
    for k in range(1, half + 1):
        from_up = owners[(at - k) % n] * rows
        from_down = owners[(at + k) % n] * rows
        if 2 * k == n:
            cut = rows // 2
            up, down = up[:cut], down[cut:]
            from_down = from_down + cut
        up = lax.ppermute(up, "sp", ahead)
        down = lax.ppermute(down, "sp", back)
        whole = lax.dynamic_update_slice(whole, up, (from_up, 0))
        whole = lax.dynamic_update_slice(whole, down, (from_down, 0))
    return whole


def on_device(
    residual,
    small_value_inputs,
    large_value_inputs,
    small_gate_inputs,
    large_gate_inputs,
    state_projections,
    small_step_inputs,
    large_step_inputs,
    small_decay_offsets,
    large_decay_offsets,
    small_decay_rates,
    large_decay_rates,
    small_filter_taps,
    large_filter_taps,
    state_filter_taps,
    small_head_gains,
    large_head_gains,
    small_output_projection,
    large_output_projection,
    channel_norm_gain,
    gate_matrix,
    up_matrix,
    down_matrix,
):
    n = lax.axis_size("sp")
    me = lax.axis_index("sp")
    margin = state_filter_taps.shape[0] - 1
    length, w1 = small_value_inputs.shape
    w2 = large_value_inputs.shape[1]
    state = state_projections.shape[2]
    planes = state_projections.shape[1] * state
    units = gate_matrix.shape[1]
    flat = state_projections.reshape(length, planes)
    series = jnp.concatenate([small_value_inputs, large_value_inputs, flat], axis=1)
    prior = lax.ppermute(
        series[length - margin :], "sp", [(i, i + 1) for i in range(n - 1)]
    )
    pack = jnp.concatenate([gate_matrix, up_matrix, down_matrix.T], axis=1)
    pack, prior = lax.optimization_barrier((pack, prior))
    whole = ring_gather(pack)

    taps = jnp.concatenate(
        [small_filter_taps, large_filter_taps, state_filter_taps.reshape(margin + 1, planes)], axis=1
    )
    conv = causal_conv(series, prior, taps)
    maps = conv[:, w1 + w2 :].astype(BF)
    keys1, reads1, keys2, reads2 = (maps[:, i * state : (i + 1) * state] for i in range(4))

    heads1 = small_decay_rates.shape[0]
    step = jax.nn.softplus(
        jnp.concatenate([small_step_inputs, large_step_inputs], axis=1).astype(F32)
    )
    rates = jnp.concatenate([small_decay_rates, large_decay_rates])
    offsets = jnp.concatenate([small_decay_offsets, large_decay_offsets], axis=1)
    log_decay = -jnp.exp(rates)[None, :] * step + offsets
    lower = jnp.tril(jnp.ones((length, length), F32))
    within = jnp.dot(lower, log_decay, precision=HIGH)

    outs1, final1 = local_heads(conv[:, :w1], step[:, :heads1], within[:, :heads1], keys1, reads1)
    outs2, final2 = local_heads(
        conv[:, w1 : w1 + w2], step[:, heads1:], within[:, heads1:], keys2, reads2
    )
    heads = rates.shape[0]
    total = jnp.exp(within[-1])
    row = jnp.pad(total[None, :], ((0, 15), (0, state - heads)))
    sent = jnp.concatenate([final1, final2, row], axis=0).astype(BF)
    gathered = lax.all_gather(sent, "sp").astype(F32)
    states1 = gathered[:, :w1].reshape(n, heads1, w1 // heads1, state)
    states2 = gathered[:, w1 : w1 + w2].reshape(n, heads - heads1, w2 // (heads - heads1), state)
    totals = gathered[:, w1 + w2, :heads]
    carry1, carry2 = jnp.zeros_like(states1[0]), jnp.zeros_like(states2[0])
    for hop in range(n - 1):
        factor1 = totals[hop, :heads1][:, None, None]
        factor2 = totals[hop, heads1:][:, None, None]
        carry1 = jnp.where(hop < me, carry1 * factor1 + states1[hop], carry1)
        carry2 = jnp.where(hop < me, carry2 * factor2 + states2[hop], carry2)
    carry1, carry2 = carry1.reshape(w1, state), carry2.reshape(w2, state)

    heads_small = finish_heads(
        outs1, carry1, within[:, :heads1], reads1, small_gate_inputs, small_head_gains
    )
    heads_large = finish_heads(
        outs2, carry2, within[:, heads1:], reads2, large_gate_inputs, large_head_gains
    )
    mixed = (
        jnp.dot(heads_small, small_output_projection, preferred_element_type=F32)
        + jnp.dot(heads_large, large_output_projection, preferred_element_type=F32)
    ).astype(BF)
    mixed = lax.psum_scatter(
        mixed,
        "tp",
        scatter_dimension=0,
        tiled=True,
    ).astype(F32)
    middle = (residual.astype(F32) + mixed).astype(BF)
    normed = row_norm(middle, channel_norm_gain)
    normed_all = lax.all_gather(normed, "tp", axis=0, tiled=True)
    gate = jnp.dot(normed_all, whole[:, :units], preferred_element_type=F32)
    up = jnp.dot(normed_all, whole[:, units : 2 * units], preferred_element_type=F32)
    hidden = (jax.nn.silu(gate) * up).astype(BF)
    partial = lax.dot_general(
        hidden, whole[:, 2 * units :], (((1,), (1,)), ((), ())), preferred_element_type=F32
    )
    down = lax.psum_scatter(
        partial.astype(BF), "tp", scatter_dimension=0, tiled=True
    ).astype(F32)
    return (middle.astype(F32) + down).astype(BF)


def solution(mesh):
    in_specs = (
        P(("sp", "tp"), None),
        P("sp", "tp"),
        P("sp", "tp"),
        P("sp", "tp"),
        P("sp", "tp"),
        P("sp", None, None),
        P("sp", "tp"),
        P("sp", "tp"),
        P("sp", "tp"),
        P("sp", "tp"),
        P("tp"),
        P("tp"),
        P(None, "tp"),
        P(None, "tp"),
        P(),
        P("tp"),
        P("tp"),
        P("tp", None),
        P("tp", None),
        P(),
        P("sp", "tp"),
        P("sp", "tp"),
        P("tp", "sp"),
    )

    return jax.shard_map(
        on_device,
        mesh=mesh,
        in_specs=in_specs,
        out_specs=P(("sp", "tp"), None),
        check_vma=False,
    )
```
